32 devices in a mesh: ep: 8 (over z, y), tp: 4 (over x, core).
Axes of the slice: x: 2, y: 2, z: 4, core: 2. Of those that a mesh axis runs over, the one named last changes fastest.
Arguments:
- pool_input: bfloat16 [12288, 2048], P('ep', 'tp'), may hold values from -6 to 6
- group_mix: bfloat16 [4, 512, 512], P('tp'), may hold values from -0.25 to 0.25
- group_scale: float32 [2048], P('tp'), may hold values from 0.1 to 1.9
- out_proj: bfloat16 [2048, 2048], replicated, may hold values from -0.125 to 0.125
- moe_input: bfloat16 [4096, 2048], P(('ep', 'tp')), may hold values from -6 to 6
- norm_gain: float32 [2048], replicated, may hold values from 0.1 to 1.9
- expert_ids: int32 [4096, 2], P(('ep', 'tp')), may hold values from 0 to 31, all different within a row; in each aligned block of 128 rows (0 to 127, 128 to 255, ...) at most 16 rows name the same one
- expert_scores: float32 [4096, 2], P(('ep', 'tp')), may hold values from 0.1 to 1
- gate_proj: bfloat16 [32, 2048, 1024], P(('ep', 'tp')), may hold values from -0.125 to 0.125
- up_proj: bfloat16 [32, 2048, 1024], P(('ep', 'tp')), may hold values from -0.125 to 0.125
- down_proj: bfloat16 [32, 1024, 2048], P(('ep', 'tp')), may hold values from -0.1875 to 0.1875
Outputs:
- mixed_tokens: bfloat16 [12288, 2048], P(('ep', 'tp'))
- mixed_experts: bfloat16 [4096, 2048], P(('ep', 'tp'))
The draws below stay inside these ranges and needn't reach their ends.
Inputs may be any that keep to these rules, and one draw needn't show every extreme that they name: `expert_ids`: each row names 2 different experts. Within the 128 rows of one device (aligned blocks) no expert is named by more than 16 rows, a bound that some block reaches of some device.
All inputs are finite; a program needn't handle non-finite values.
Results may differ from the reference program's by a relative error of at most 0.012.
Values may be sent and summed in bfloat16 or wider, within the bound.
No kernel may reach another device: no remote copies, remote signals or barrier semaphores. Data moves between devices by JAX's collectives and lax.ppermute only.
A program may use at most 128 MiB of HBM per device.

```python
import math
import jax
import jax.numpy as jnp
import numpy as np
from jax import lax

D = 2048
GROUPS = 4
FF = 1024
TOPK = 2
TOK_B_DEV = 128
GW = 512
TOKENS_A = 12288
TOKENS_B = 4096
EXPERTS = 32
CAP = 16
N_EP = 8
N_TP = 4


def block_levels(own_key, shape, cuts, smallest, largest):
    factor_of = 1.0
    for axis_at, blocks in cuts:
        draws = jax.random.uniform(jax.random.fold_in(jax.random.fold_in(own_key, 6), axis_at), (blocks,), jnp.float32, smallest / len(cuts), largest / len(cuts))
        factor_of = factor_of * jnp.repeat(jnp.exp(draws), shape[axis_at] // blocks).reshape((-1,) + (1,) * (len(shape) - 1 - axis_at))
    return factor_of


def shared_out(stream_key, own, number, rows, number_of, top, bound, skew):
    order = jax.random.permutation(stream_key, number_of)
    crowded, common = load_shares(number_of, rows * top, bound, skew, True), load_shares(number_of, rows * top, bound, skew, False)
    places = jnp.arange(number_of)

    def named(lengths, offset_by):
        used = int((lengths > 0).sum())
        fixed = max(1, used // 4)
        passed = fixed + (places - fixed + offset_by * (used - fixed)) % max(1, number_of - fixed)
        return jnp.zeros((number_of,), jnp.int32).at[order[jnp.where(places < fixed, places, passed)]].set(jnp.asarray(lengths, jnp.int32))

    lengths = jnp.where(number % 4 == 0, named(crowded, number // 4), named(common, number - number // 4 - 1))
    mixed = jax.random.permutation(jax.random.fold_in(own, 3), number_of)
    giver, receiver = mixed[0:number_of // 2 * 2:2], mixed[1:number_of // 2 * 2:2]
    margin = jnp.minimum(lengths[giver] - 1, bound - lengths[receiver]) // 2
    margin = jnp.where((giver == order[0]) | (receiver == order[0]) | (lengths[receiver] == 0), 0, jnp.maximum(margin, 0))
    passed = jax.random.randint(jax.random.fold_in(own, 4), (number_of // 2,), 0, 1 << 20) % (margin + 1)
    lengths = lengths.at[giver].add(-passed).at[receiver].add(passed)
    labels = jnp.searchsorted(jnp.cumsum(lengths), jnp.arange(rows * top), side="right").astype(jnp.int32)
    listing = labels.reshape(top, rows).T
    listing = listing[jax.random.permutation(jax.random.fold_in(own, 1), rows)]
    offset_by = jax.random.randint(jax.random.fold_in(own, 2), (rows, 1), 0, top)
    return jnp.take_along_axis(listing, (jnp.arange(top)[None, :] + offset_by) % top, axis=1)


def load_shares(count, total, limit, skew, full):
    loads = [(1 << 20) // math.isqrt(rank ** skew) + 1 for rank in range(1, count + 1)]
    largest = limit if full else min(limit, max(-(-total // count), total * loads[0] // sum(loads)))
    least = 1 if total - largest >= count - 1 else 0
    given, spare = [largest] + [least] * (count - 1), total - largest - least * (count - 1)
    while spare > 0:
        candidates = [i for i in range(1, count) if given[i] < largest] or [i for i in range(1, count) if given[i] < limit]
        whole, remaining = sum([loads[i] for i in candidates]), spare
        for i in candidates:
            extra = min(limit - given[i], max(1, remaining * loads[i] // whole), spare)
            given[i] = given[i] + extra
            spare = spare - extra
    return np.array(given)


def normal_values(stream_key, extent, deviation, limit, cuts=(), kind=jnp.bfloat16):
    values = deviation * jax.random.normal(stream_key, extent, jnp.float32)
    if cuts:
        values = values * block_levels(stream_key, extent, cuts, -0.22, 0.18)
    return jnp.clip(values, -limit, limit).astype(kind)


def setup_inputs(seed: int = 0) -> dict:
    arg_keys = jax.random.split(jax.random.key(seed), 12)
    pool_input = normal_values(arg_keys[0], (TOKENS_A, D), 1.0, 6.0, ((0, 8), (1, 4)))
    group_mix = normal_values(arg_keys[1], (GROUPS, GW, GW), GW ** -0.5, 0.25, ((0, 4),))
    group_scale = jnp.clip(1.0 + 0.18 * jax.random.normal(arg_keys[2], (D,), jnp.float32), 0.1, 1.9)
    out_proj = normal_values(arg_keys[3], (D, D), D ** -0.5, 0.125)
    moe_input = normal_values(arg_keys[4], (TOKENS_B, D), 1.0, 6.0, ((0, 32),))
    norm_gain = jnp.clip(1.0 + 0.18 * jax.random.normal(arg_keys[5], (D,), jnp.float32), 0.1, 1.9)
    expert_ids_keys = jax.random.split(jax.random.fold_in(arg_keys[6], 1), TOKENS_B // TOK_B_DEV)
    expert_ids_turns = jax.random.permutation(jax.random.fold_in(arg_keys[6], 3), TOKENS_B // TOK_B_DEV)
    expert_ids = jax.vmap(lambda own, number: shared_out(jax.random.fold_in(arg_keys[6], 2), own, number, TOK_B_DEV, EXPERTS, TOPK, CAP, 2))(expert_ids_keys, expert_ids_turns).reshape((TOKENS_B, TOPK))
    expert_scores = jnp.clip(jnp.exp(math.log(1.0) - 2.3025851 * jax.random.uniform(arg_keys[7], (TOKENS_B, TOPK), jnp.float32) ** block_levels(arg_keys[7], (TOKENS_B, TOPK), ((0, 32),), -0.2, 0.2)), 0.1, 1.0)
    gate_proj = normal_values(arg_keys[8], (EXPERTS, D, FF), D ** -0.5, 0.125, ((0, 32),))
    up_proj = normal_values(arg_keys[9], (EXPERTS, D, FF), D ** -0.5, 0.125, ((0, 32),))
    down_proj = normal_values(arg_keys[10], (EXPERTS, FF, D), FF ** -0.5, 0.1875, ((0, 32),))
    return dict(pool_input=pool_input, group_mix=group_mix, group_scale=group_scale, out_proj=out_proj, moe_input=moe_input, norm_gain=norm_gain, expert_ids=expert_ids, expert_scores=expert_scores, gate_proj=gate_proj, up_proj=up_proj, down_proj=down_proj)


epsilon = 1e-06

def pool_reference(pool_input, group_mix, group_scale, out_proj):
    total_rows, model_width = pool_input.shape
    group_count, group_width = (group_mix.shape[0], group_mix.shape[1])
    values = pool_input.astype(jnp.float32)
    running = jnp.concatenate([jnp.zeros((1, model_width), jnp.float32), jnp.cumsum(values, axis=0)], axis=0)
    position = jnp.arange(total_rows)
    pieces = []
    for group_id in range(group_count):
        window_len = 2 ** (group_id + 1)
        col_lower = group_id * group_width
        col_upper = col_lower + group_width
        start_row = jnp.maximum(position + 1 - window_len, 0)
        counted = jnp.minimum(position + 1, window_len).astype(jnp.float32)
        window_sum = running[1:, col_lower:col_upper] - running[start_row, col_lower:col_upper]
        pooled = (window_sum / counted[:, None] - values[:, col_lower:col_upper]).astype(jnp.bfloat16)
        grouped = jnp.dot(pooled, group_mix[group_id], preferred_element_type=jnp.float32)
        pieces.append((grouped * group_scale[col_lower:col_upper]).astype(jnp.bfloat16))
    hidden = jnp.concatenate(pieces, axis=1)
    return jnp.dot(hidden, out_proj, preferred_element_type=jnp.float32).astype(jnp.bfloat16)

def expert_reference(moe_input, norm_gain, expert_ids, expert_scores, gate_proj, up_proj, down_proj):
    total_rows, model_width = moe_input.shape
    top_count = expert_ids.shape[1]
    experts_all = gate_proj.shape[0]
    span_rows = N_EP * N_TP * CAP
    values = moe_input.astype(jnp.float32)
    normed = (values * lax.rsqrt(lax.optimization_barrier(jnp.mean(values * values, axis=1, keepdims=True)) + epsilon) * norm_gain).astype(jnp.bfloat16)
    flat_ids = expert_ids.reshape(-1).astype(jnp.int32)
    order_idx = jnp.argsort(flat_ids, stable=True).astype(jnp.int32)
    sorted_ids = flat_ids[order_idx]
    counts = lax.optimization_barrier(jnp.sum((flat_ids[:, None] == jnp.arange(experts_all).astype(jnp.int32)[None, :]).astype(jnp.int32), axis=0)).astype(jnp.int32)
    starts = (jnp.cumsum(counts) - counts).astype(jnp.int32)
    sorted_rows = jnp.concatenate([normed[order_idx // top_count], jnp.zeros((span_rows, model_width), jnp.bfloat16)], axis=0)

    def one_expert(expert_idx):
        rows_in = lax.dynamic_slice_in_dim(sorted_rows, starts[expert_idx], span_rows, 0)
        gate_part = jnp.dot(rows_in, gate_proj[expert_idx], preferred_element_type=jnp.float32)
        up_part = jnp.dot(rows_in, up_proj[expert_idx], preferred_element_type=jnp.float32)
        active = (jax.nn.silu(gate_part) * up_part).astype(jnp.bfloat16)
        return jnp.dot(active, down_proj[expert_idx], preferred_element_type=jnp.float32).astype(jnp.bfloat16)
    outputs = lax.map(one_expert, jnp.arange(experts_all).astype(jnp.int32))
    slot_rank = (jnp.arange(flat_ids.shape[0]).astype(jnp.int32) - starts[sorted_ids]).astype(jnp.int32)
    sorted_out = outputs[sorted_ids, slot_rank]
    per_assign = jnp.zeros((flat_ids.shape[0], model_width), jnp.bfloat16).at[order_idx].set(sorted_out)
    picked = per_assign.astype(jnp.float32).reshape(total_rows, top_count, model_width)
    scores = expert_scores.astype(jnp.float32)
    weights = scores / lax.optimization_barrier(jnp.sum(scores, axis=1, keepdims=True))
    return lax.optimization_barrier(jnp.sum(picked * weights[:, :, None], axis=1)).astype(jnp.bfloat16)

def reference(pool_input, group_mix, group_scale, out_proj, moe_input, norm_gain, expert_ids, expert_scores, gate_proj, up_proj, down_proj):
    mixed_tokens = pool_reference(pool_input, group_mix, group_scale, out_proj)
    mixed_experts = expert_reference(moe_input, norm_gain, expert_ids, expert_scores, gate_proj, up_proj, down_proj)
    return (mixed_tokens, mixed_experts)
```

```python
import functools

import jax
import jax.numpy as jnp
from jax import lax
from jax.experimental import pallas as pl
from jax.experimental.pallas import tpu as pltpu
from jax.sharding import Mesh
from jax.sharding import PartitionSpec as P

epsilon = 1e-06
HALO = 16
MIB = 1 << 20


def whole(memory_space=pltpu.VMEM):
    return pl.BlockSpec(memory_space=memory_space)


def call(kernel, out_shape, flops, moved, limit=12, **options):
    return pl.pallas_call(
        kernel,
        out_shape=out_shape,
        compiler_params=pltpu.CompilerParams(vmem_limit_bytes=limit * MIB),
        cost_estimate=pl.CostEstimate(flops=flops, bytes_accessed=moved, transcendentals=0),
        **options,
    )


def peer(index, step, count):
    if count & (count - 1) == 0:
        return index ^ step
    return (index + step) % count


def source_of(index, step, count):
    if count & (count - 1) == 0:
        return index ^ step
    return (index - step) % count


def norm_kernel(x_ref, gain_ref, out_ref):
    values = x_ref[...].astype(jnp.float32)
    mean = jnp.mean(values * values, axis=1, keepdims=True)
    out_ref[...] = (values * lax.rsqrt(mean + epsilon) * gain_ref[...]).astype(out_ref.dtype)


def norm_rows(moe_input, norm_gain):
    rows, width = moe_input.shape
    return call(
        norm_kernel,
        jax.ShapeDtypeStruct((rows, width), jnp.bfloat16),
        rows * width * 8,
        rows * width * 4,
        in_specs=[whole(), whole()],
        out_specs=whole(),
    )(moe_input, norm_gain.reshape(1, width))


def pick_rows(first, second, rows, slots):
    slot = lax.broadcasted_iota(jnp.int32, (slots, rows.shape[0]), 0)
    held = (slot == first) | (slot == second)
    return jnp.dot(
        jnp.where(held, 1.0, 0.0).astype(jnp.bfloat16), rows, preferred_element_type=jnp.float32
    ).astype(jnp.bfloat16)


def route_kernel(capacity, experts, slots, ids_ref, scores_ref, rows_ref, meta_ref, out_ref):
    tokens = ids_ref.shape[1]
    ids = ids_ref[...]
    scores = scores_ref[...]
    expert = lax.broadcasted_iota(jnp.int32, (experts, tokens), 0)
    earlier = lax.broadcasted_iota(jnp.int32, (tokens, tokens), 0) < lax.broadcasted_iota(
        jnp.int32, (tokens, tokens), 1
    )
    before = jnp.where(earlier, 1.0, 0.0).astype(jnp.bfloat16)
    used = jnp.zeros((experts, 1), jnp.float32)
    places = []
    for choice in range(2):
        chosen = jnp.where(expert == ids[choice : choice + 1, :], 1.0, 0.0)
        rank = used + jnp.dot(
            chosen.astype(jnp.bfloat16), before, preferred_element_type=jnp.float32
        )
        rank = jnp.sum(chosen * rank, axis=0, keepdims=True)
        used = used + jnp.sum(chosen, axis=1, keepdims=True)
        places.append(ids[choice : choice + 1, :] * capacity + rank.astype(jnp.int32))
    total = scores[0:1, :] + scores[1:2, :]
    meta_ref[...] = jnp.zeros_like(meta_ref)
    for choice in range(2):
        meta_ref[choice : choice + 1, :] = places[choice].astype(jnp.float32)
        meta_ref[2 + choice : 3 + choice, :] = scores[choice : choice + 1, :] / total
    base = lax.axis_index("half") * slots
    out_ref[...] = pick_rows(places[0] - base, places[1] - base, rows_ref[...], slots)


def route(expert_ids, expert_scores, normed, capacity, experts, slots):
    tokens, width = normed.shape
    return call(
        functools.partial(route_kernel, capacity, experts, slots),
        (
            jax.ShapeDtypeStruct((8, tokens), jnp.float32),
            jax.ShapeDtypeStruct((slots, width), jnp.bfloat16),
        ),
        2 * slots * tokens * width,
        2 * (slots + tokens) * width,
        in_specs=[whole(), whole(), whole()],
        out_specs=(whole(), whole()),
    )(expert_ids.T, expert_scores.T, normed)


def pick_kernel(slots, meta_ref, rows_ref, out_ref):
    base = lax.axis_index("half") * slots
    first = meta_ref[0:1, :].astype(jnp.int32) - base
    second = meta_ref[1:2, :].astype(jnp.int32) - base
    out_ref[...] = pick_rows(first, second, rows_ref[...], slots)


def pick(meta, rows, slots):
    tokens, width = rows.shape
    return call(
        functools.partial(pick_kernel, slots),
        jax.ShapeDtypeStruct((slots, width), jnp.bfloat16),
        2 * slots * tokens * width,
        2 * (slots + tokens) * width,
        in_specs=[whole(), whole()],
        out_specs=whole(),
    )(meta, rows)


def weighted_sum(meta_ref, rows_ref):
    slots, tokens = rows_ref.shape[0], meta_ref.shape[1]
    base = lax.axis_index("half") * slots
    slot = lax.broadcasted_iota(jnp.int32, (slots, tokens), 0)
    spread = jnp.zeros((slots, tokens), jnp.float32)
    for choice in range(2):
        place = meta_ref[choice : choice + 1, :].astype(jnp.int32) - base
        spread = spread + jnp.where(slot == place, meta_ref[2 + choice : 3 + choice, :], 0.0)
    high = spread.astype(jnp.bfloat16)
    low = (spread - high.astype(jnp.float32)).astype(jnp.bfloat16)
    over = (((0,), (0,)), ((), ()))
    rows = rows_ref[...]
    return lax.dot_general(high, rows, over, preferred_element_type=jnp.float32) + lax.dot_general(
        low, rows, over, preferred_element_type=jnp.float32
    )


def partial_kernel(meta_ref, rows_ref, out_ref):
    out_ref[...] = weighted_sum(meta_ref, rows_ref).astype(out_ref.dtype)


def final_kernel(meta_ref, rows_ref, other_ref, out_ref):
    total = weighted_sum(meta_ref, rows_ref) + other_ref[...].astype(jnp.float32)
    out_ref[...] = total.astype(out_ref.dtype)


def combine(meta, rows, other=None):
    slots, width = rows.shape
    tokens = meta.shape[1]
    others = () if other is None else (other,)
    return call(
        partial_kernel if other is None else final_kernel,
        jax.ShapeDtypeStruct((tokens, width), jnp.bfloat16),
        4 * slots * tokens * width,
        2 * (slots + tokens) * width,
        in_specs=[whole()] * (2 + len(others)),
        out_specs=whole(),
    )(meta, rows, *others)


def expert_kernel(tile, x_ref, gate_hbm, up_hbm, down_hbm, out_ref, gate, up, down, total, arrived):
    steps = gate.shape[0]
    copies = []
    for step in range(steps):
        part = pl.ds(step * tile, tile)
        copies.append(
            (
                pltpu.make_async_copy(gate_hbm.at[0, :, part], gate.at[step], arrived.at[step, 0]),
                pltpu.make_async_copy(up_hbm.at[0, :, part], up.at[step], arrived.at[step, 1]),
                pltpu.make_async_copy(down_hbm.at[0, part, :], down.at[step], arrived.at[step, 2]),
            )
        )
        for copy in copies[-1]:
            copy.start()
    x = x_ref[...]
    for step in range(steps):
        copies[step][0].wait()
        gated = jnp.dot(x, gate[step], preferred_element_type=jnp.float32)
        copies[step][1].wait()
        raised = jnp.dot(x, up[step], preferred_element_type=jnp.float32)
        active = (gated / (1.0 + jnp.exp(-gated)) * raised).astype(jnp.bfloat16)
        copies[step][2].wait()
        share = jnp.dot(active, down[step], preferred_element_type=jnp.float32)
        if step == 0:
            total[...] = share
        elif step < steps - 1:
            total[...] += share
        else:
            out_ref[...] = (total[...] + share).astype(out_ref.dtype)


def experts_on(rows, gate_proj, up_proj, down_proj):
    count, width = rows.shape
    hidden = gate_proj.shape[2]
    tile = 256
    steps = hidden // tile
    return call(
        functools.partial(expert_kernel, tile),
        jax.ShapeDtypeStruct((count, width), jnp.bfloat16),
        6 * count * width * hidden,
        6 * width * hidden + 4 * count * width,
        limit=26,
        in_specs=[whole()] + [whole(pltpu.HBM)] * 3,
        out_specs=whole(),
        scratch_shapes=[
            pltpu.VMEM((steps, width, tile), jnp.bfloat16),
            pltpu.VMEM((steps, width, tile), jnp.bfloat16),
            pltpu.VMEM((steps, tile, width), jnp.bfloat16),
            pltpu.VMEM((count, width), jnp.float32),
            pltpu.SemaphoreType.DMA((steps, 3)),
        ],
    )(rows, gate_proj, up_proj, down_proj)


def pool_kernel(count, tile, halo_ref, x_ref, mix_ref, scale_ref, *refs):
    outs, extended = refs[:count], refs[count]
    rows = x_ref.shape[0]
    extended[0:HALO, :] = halo_ref[...]
    extended[HALO:, :] = x_ref[...]
    group = lax.axis_index("tp")
    first = (lax.axis_index("half") * lax.axis_size("inner") + lax.axis_index("inner")) * rows
    window = jnp.left_shift(jnp.int32(2), group)
    row = lax.broadcasted_iota(jnp.int32, (tile, tile + HALO), 0)
    column = lax.broadcasted_iota(jnp.int32, (tile, tile + HALO), 1) - HALO
    inside = (column <= row) & (column > row - window)
    band = jnp.where(inside, 1.0, 0.0).astype(jnp.bfloat16)
    share = rows // count
    for step in range(count):
        start = peer(group, step, count) * share

        for piece in range(share // tile):
            at = pl.multiple_of(start + piece * tile, tile)
            trailing = jnp.dot(
                band, extended[pl.ds(at, tile + HALO), :], preferred_element_type=jnp.float32
            )
            position = first + at + lax.broadcasted_iota(jnp.int32, (tile, 1), 0)
            counted = jnp.minimum(position + 1, window).astype(jnp.float32)
            own = x_ref[pl.ds(at, tile), :].astype(jnp.float32)
            pooled = (trailing / counted - own).astype(jnp.bfloat16)
            grouped = jnp.dot(pooled, mix_ref[0], preferred_element_type=jnp.float32)
            outs[step][piece * tile : (piece + 1) * tile, :] = (grouped * scale_ref[...]).astype(
                jnp.bfloat16
            )


def pool(halo, pool_input, group_mix, group_scale, count):
    rows, width = pool_input.shape
    share = rows // count
    return call(
        functools.partial(pool_kernel, count, 128),
        [jax.ShapeDtypeStruct((share, width), jnp.bfloat16)] * count,
        2 * rows * width * width,
        4 * rows * width,
        in_specs=[whole()] * 4,
        out_specs=[whole()] * count,
        scratch_shapes=[pltpu.VMEM((rows + HALO, width), jnp.bfloat16)],
    )(halo, pool_input, group_mix, group_scale.reshape(1, width))


def project_kernel(count, *refs):
    pieces, weight_ref, out_ref = refs[:count], refs[count], refs[count + 1]
    width = pieces[0].shape[1]
    total = None
    for step in range(count):
        at = pl.multiple_of(source_of(lax.axis_index("tp"), step, count) * width, width)
        share = jnp.dot(
            pieces[step][...], weight_ref[pl.ds(at, width), :], preferred_element_type=jnp.float32
        )
        total = share if total is None else total + share
    out_ref[...] = total.astype(out_ref.dtype)


def project(pieces, out_proj):
    rows, width = pieces[0].shape
    depth, columns = out_proj.shape
    tile = 512
    return call(
        functools.partial(project_kernel, len(pieces)),
        jax.ShapeDtypeStruct((rows, columns), jnp.bfloat16),
        2 * rows * depth * columns,
        2 * depth * columns + 2 * rows * (depth + columns),
        grid=(columns // tile,),
        in_specs=[pl.BlockSpec((rows, width), lambda j: (0, 0))] * len(pieces)
        + [pl.BlockSpec((depth, tile), lambda j: (0, j))],
        out_specs=pl.BlockSpec((rows, tile), lambda j: (0, j)),
    )(*pieces, out_proj)


def body(
    pool_input,
    group_mix,
    group_scale,
    out_proj,
    moe_input,
    norm_gain,
    expert_ids,
    expert_scores,
    gate_proj,
    up_proj,
    down_proj,
):
    n_half, n_inner, n_tp = (lax.axis_size(axis) for axis in ("half", "inner", "tp"))
    tokens, width = moe_input.shape
    members = n_inner * n_tp
    experts = n_half * members
    capacity = 2 * tokens * expert_ids.shape[1] // experts
    slots = members * capacity
    pool_rows = pool_input.shape[0]

    def across(value):
        return lax.ppermute(value, "half", [(0, 1), (1, 0)])

    def spread(rows):
        out = lax.all_to_all(
            rows.reshape(members, capacity, width), ("inner", "tp"), 0, 0, tiled=True
        )
        return out.reshape(slots, width)

    halo = lax.ppermute(
        pool_input[pool_rows - HALO :],
        ("half", "inner"),
        [(source, source + 1) for source in range(n_half * n_inner - 1)],
    )
    normed = norm_rows(moe_input, norm_gain)
    other_rows = across(normed)
    meta, own_slots = route(expert_ids, expert_scores, normed, capacity, experts, slots)
    other_meta = across(meta)
    own_in = spread(own_slots)

    hidden = pool(halo, pool_input, group_mix, group_scale, n_tp)
    other_rows, own_in, hidden = lax.optimization_barrier((other_rows, own_in, hidden))
    pieces = [hidden[0]] + [
        lax.ppermute(hidden[step], "tp", [(s, peer(s, step, n_tp)) for s in range(n_tp)])
        for step in range(1, n_tp)
    ]

    other_in = spread(pick(other_meta, other_rows, slots))
    own_out = experts_on(own_in, gate_proj, up_proj, down_proj)
    own_out, other_in = lax.optimization_barrier((own_out, other_in))
    other_out = experts_on(other_in, gate_proj, up_proj, down_proj)
    other_back = spread(other_out)
    mixed_tokens = project(pieces, out_proj)
    mixed_tokens, other_back = lax.optimization_barrier((mixed_tokens, other_back))
    partial = combine(other_meta, other_back)
    own_out, partial = lax.optimization_barrier((own_out, partial))
    partial_back = across(partial)
    own_back = spread(own_out)
    mixed_experts = combine(meta, own_back, partial_back)
    return (mixed_tokens, mixed_experts)


def solution(mesh):
    n_ep, n_tp = mesh.shape["ep"], mesh.shape["tp"]
    split = Mesh(mesh.devices.reshape(2, n_ep // 2, n_tp), ("half", "inner", "tp"))
    ep = ("half", "inner")
    every = ("half", "inner", "tp")
    placed = (
        P(ep, "tp"),
        P("tp", None, None),
        P("tp"),
        P(),
        P(every, None),
        P(),
        P(every, None),
        P(every, None),
        P(every, None, None),
        P(every, None, None),
        P(every, None, None),
    )
    return jax.shard_map(
        body,
        mesh=split,
        in_specs=placed,
        out_specs=(P(every, None), P(every, None)),
        check_vma=False,
    )
```

```python
import functools

import jax
import jax.numpy as jnp
from jax import lax
from jax.experimental import pallas as pl
from jax.experimental.pallas import tpu as pltpu
from jax.sharding import Mesh
from jax.sharding import PartitionSpec as P


epsilon = 1e-06
HALO = 16
MIB = 1 << 20


def whole(memory_space=pltpu.VMEM):
    return pl.BlockSpec(memory_space=memory_space)


def block(array):
    return pl.BlockSpec(array.shape, lambda j: (0,) * array.ndim)


def in_hbm(array):
    return pltpu.with_memory_space_constraint(array, pltpu.HBM)


def call(kernel, out_shape, flops, moved, limit=12, **options):
    return pl.pallas_call(
        kernel,
        out_shape=out_shape,
        compiler_params=pltpu.CompilerParams(vmem_limit_bytes=limit * MIB),
        cost_estimate=pl.CostEstimate(flops=flops, bytes_accessed=moved, transcendentals=0),
        **options,
    )


def peer(index, step, count):
    if count & (count - 1) == 0:
        return index ^ step
    return (index + step) % count


def source_of(index, step, count):
    if count & (count - 1) == 0:
        return index ^ step
    return (index - step) % count


def norm_kernel(x_ref, gain_ref, out_ref):
    values = x_ref[...].astype(jnp.float32)
    mean = jnp.mean(values * values, axis=1, keepdims=True)
    out_ref[...] = (values * lax.rsqrt(mean + epsilon) * gain_ref[...]).astype(out_ref.dtype)


def norm_rows(moe_input, norm_gain):
    rows, width = moe_input.shape
    return call(
        norm_kernel,
        jax.ShapeDtypeStruct((rows, width), jnp.bfloat16),
        rows * width * 8,
        rows * width * 4,
        grid=(1,),
        in_specs=[block(moe_input), pl.BlockSpec((1, width), lambda j: (0, 0))],
        out_specs=whole(),
    )(in_hbm(moe_input), in_hbm(norm_gain.reshape(1, width)))


def pick_rows(first, second, rows, slots):
    slot = lax.broadcasted_iota(jnp.int32, (slots, rows.shape[0]), 0)
    held = (slot == first) | (slot == second)
    return jnp.dot(
        jnp.where(held, 1.0, 0.0).astype(jnp.bfloat16), rows, preferred_element_type=jnp.float32
    ).astype(jnp.bfloat16)


def route_kernel(capacity, experts, slots, ids_ref, scores_ref, rows_ref, meta_ref, out_ref):
    tokens = ids_ref.shape[1]
    ids = ids_ref[...]
    scores = scores_ref[...]
    expert = lax.broadcasted_iota(jnp.int32, (experts, tokens), 0)
    earlier = lax.broadcasted_iota(jnp.int32, (tokens, tokens), 0) < lax.broadcasted_iota(
        jnp.int32, (tokens, tokens), 1
    )
    before = jnp.where(earlier, 1.0, 0.0).astype(jnp.bfloat16)
    used = jnp.zeros((experts, 1), jnp.float32)
    places = []
    for choice in range(2):
        chosen = jnp.where(expert == ids[choice : choice + 1, :], 1.0, 0.0)
        rank = used + jnp.dot(
            chosen.astype(jnp.bfloat16), before, preferred_element_type=jnp.float32
        )
        rank = jnp.sum(chosen * rank, axis=0, keepdims=True)
        used = used + jnp.sum(chosen, axis=1, keepdims=True)
        places.append(ids[choice : choice + 1, :] * capacity + rank.astype(jnp.int32))
    total = scores[0:1, :] + scores[1:2, :]
    meta_ref[...] = jnp.zeros_like(meta_ref)
    for choice in range(2):
        meta_ref[choice : choice + 1, :] = places[choice].astype(jnp.float32)
        meta_ref[2 + choice : 3 + choice, :] = scores[choice : choice + 1, :] / total
    base = lax.axis_index("half") * slots
    out_ref[...] = pick_rows(places[0] - base, places[1] - base, rows_ref[...], slots)


def route(expert_ids, expert_scores, normed, capacity, experts, slots):
    tokens, width = normed.shape
    return call(
        functools.partial(route_kernel, capacity, experts, slots),
        (
            jax.ShapeDtypeStruct((8, tokens), jnp.float32),
            jax.ShapeDtypeStruct((slots, width), jnp.bfloat16),
        ),
        2 * slots * tokens * width,
        2 * (slots + tokens) * width,
        grid=(1,),
        in_specs=[block(expert_ids.T), block(expert_scores.T), whole()],
        out_specs=(whole(), whole()),
    )(in_hbm(expert_ids.T), in_hbm(expert_scores.T), normed)


def pick_kernel(slots, meta_ref, rows_ref, out_ref):
    base = lax.axis_index("half") * slots
    first = meta_ref[0:1, :].astype(jnp.int32) - base
    second = meta_ref[1:2, :].astype(jnp.int32) - base
    out_ref[...] = pick_rows(first, second, rows_ref[...], slots)


def pick(meta, rows, slots):
    tokens, width = rows.shape
    return call(
        functools.partial(pick_kernel, slots),
        jax.ShapeDtypeStruct((slots, width), jnp.bfloat16),
        2 * slots * tokens * width,
        2 * (slots + tokens) * width,
        in_specs=[whole(), whole()],
        out_specs=whole(),
    )(meta, rows)


def weighted_sum(meta_ref, rows_ref):
    slots, tokens = rows_ref.shape[0], meta_ref.shape[1]
    base = lax.axis_index("half") * slots
    slot = lax.broadcasted_iota(jnp.int32, (slots, tokens), 0)
    spread = jnp.zeros((slots, tokens), jnp.float32)
    for choice in range(2):
        place = meta_ref[choice : choice + 1, :].astype(jnp.int32) - base
        spread = spread + jnp.where(slot == place, meta_ref[2 + choice : 3 + choice, :], 0.0)
    high = spread.astype(jnp.bfloat16)
    low = (spread - high.astype(jnp.float32)).astype(jnp.bfloat16)
    over = (((0,), (0,)), ((), ()))
    rows = rows_ref[...]
    return lax.dot_general(high, rows, over, preferred_element_type=jnp.float32) + lax.dot_general(
        low, rows, over, preferred_element_type=jnp.float32
    )


def partial_kernel(meta_ref, rows_ref, out_ref):
    out_ref[...] = weighted_sum(meta_ref, rows_ref).astype(out_ref.dtype)


def final_kernel(meta_ref, rows_ref, other_ref, out_ref):
    total = weighted_sum(meta_ref, rows_ref) + other_ref[...].astype(jnp.float32)
    out_ref[...] = total.astype(out_ref.dtype)


def combine(meta, rows, other=None):
    slots, width = rows.shape
    tokens = meta.shape[1]
    others = () if other is None else (other,)
    return call(
        partial_kernel if other is None else final_kernel,
        jax.ShapeDtypeStruct((tokens, width), jnp.bfloat16),
        4 * slots * tokens * width,
        2 * (slots + tokens) * width,
        in_specs=[whole()] * (2 + len(others)),
        out_specs=whole(),
    )(meta, rows, *others)


def expert_kernel(tile, x_ref, gate_hbm, up_hbm, down_hbm, out_ref, gate, up, down, total, arrived):
    steps = gate.shape[0]
    copies = []
    for step in range(steps):
        part = pl.ds(step * tile, tile)
        copies.append(
            (
                pltpu.make_async_copy(gate_hbm.at[0, :, part], gate.at[step], arrived.at[step, 0]),
                pltpu.make_async_copy(up_hbm.at[0, :, part], up.at[step], arrived.at[step, 1]),
                pltpu.make_async_copy(down_hbm.at[0, part, :], down.at[step], arrived.at[step, 2]),
            )
        )
        for copy in copies[-1]:
            copy.start()
    x = x_ref[...]
    for step in range(steps):
        copies[step][0].wait()
        gated = jnp.dot(x, gate[step], preferred_element_type=jnp.float32)
        copies[step][1].wait()
        raised = jnp.dot(x, up[step], preferred_element_type=jnp.float32)
        active = (gated / (1.0 + jnp.exp(-gated)) * raised).astype(jnp.bfloat16)
        copies[step][2].wait()
        share = jnp.dot(active, down[step], preferred_element_type=jnp.float32)
        if step == 0:
            total[...] = share
        elif step < steps - 1:
            total[...] += share
        else:
            out_ref[...] = (total[...] + share).astype(out_ref.dtype)


def experts_on(rows, gate_proj, up_proj, down_proj):
    count, width = rows.shape
    hidden = gate_proj.shape[2]
    tile = 256
    steps = hidden // tile
    return call(
        functools.partial(expert_kernel, tile),
        jax.ShapeDtypeStruct((count, width), jnp.bfloat16),
        6 * count * width * hidden,
        6 * width * hidden + 4 * count * width,
        limit=26,
        in_specs=[whole()] + [whole(pltpu.HBM)] * 3,
        out_specs=whole(),
        scratch_shapes=[
            pltpu.VMEM((steps, width, tile), jnp.bfloat16),
            pltpu.VMEM((steps, width, tile), jnp.bfloat16),
            pltpu.VMEM((steps, tile, width), jnp.bfloat16),
            pltpu.VMEM((count, width), jnp.float32),
            pltpu.SemaphoreType.DMA((steps, 3)),
        ],
    )(rows, in_hbm(gate_proj), in_hbm(up_proj), in_hbm(down_proj))


def pool_kernel(count, tile, halo_ref, x_ref, mix_ref, scale_ref, *refs):
    outs, extended = refs[:count], refs[count]
    rows = x_ref.shape[0]
    extended[0:HALO, :] = halo_ref[...]
    extended[HALO:, :] = x_ref[...]
    group = lax.axis_index("tp")
    first = (lax.axis_index("half") * lax.axis_size("inner") + lax.axis_index("inner")) * rows
    window = jnp.left_shift(jnp.int32(2), group)
    row = lax.broadcasted_iota(jnp.int32, (tile, tile + HALO), 0)
    column = lax.broadcasted_iota(jnp.int32, (tile, tile + HALO), 1) - HALO
    inside = (column <= row) & (column > row - window)
    band = jnp.where(inside, 1.0, 0.0).astype(jnp.bfloat16)
    share = rows // count
    for step in range(count):
        start = peer(group, step, count) * share

        for piece in range(share // tile):
            at = pl.multiple_of(start + piece * tile, tile)
            trailing = jnp.dot(
                band, extended[pl.ds(at, tile + HALO), :], preferred_element_type=jnp.float32
            )
            position = first + at + lax.broadcasted_iota(jnp.int32, (tile, 1), 0)
            counted = jnp.minimum(position + 1, window).astype(jnp.float32)
            own = x_ref[pl.ds(at, tile), :].astype(jnp.float32)
            pooled = (trailing / counted - own).astype(jnp.bfloat16)
            grouped = jnp.dot(pooled, mix_ref[0], preferred_element_type=jnp.float32)
            outs[step][piece * tile : (piece + 1) * tile, :] = (grouped * scale_ref[...]).astype(
                jnp.bfloat16
            )


def pool(halo, pool_input, group_mix, group_scale, count):
    rows, width = pool_input.shape
    share = rows // count
    return call(
        functools.partial(pool_kernel, count, 128),
        [jax.ShapeDtypeStruct((share, width), jnp.bfloat16)] * count,
        2 * rows * width * width,
        4 * rows * width,
        grid=(1,),
        in_specs=[
            whole(),
            block(pool_input),
            block(group_mix),
            pl.BlockSpec((1, width), lambda j: (0, 0)),
        ],
        out_specs=[whole()] * count,
        scratch_shapes=[pltpu.VMEM((rows + HALO, width), jnp.bfloat16)],
    )(halo, in_hbm(pool_input), in_hbm(group_mix), in_hbm(group_scale.reshape(1, width)))


def project_kernel(count, *refs):
    pieces, weight_ref, out_ref = refs[:count], refs[count], refs[count + 1]
    width = pieces[0].shape[1]
    total = None
    for step in range(count):
        at = pl.multiple_of(source_of(lax.axis_index("tp"), step, count) * width, width)
        share = jnp.dot(
            pieces[step][...], weight_ref[pl.ds(at, width), :], preferred_element_type=jnp.float32
        )
        total = share if total is None else total + share
    out_ref[...] = total.astype(out_ref.dtype)


def project(pieces, out_proj):
    rows, width = pieces[0].shape
    depth, columns = out_proj.shape
    tile = 512
    return call(
        functools.partial(project_kernel, len(pieces)),
        jax.ShapeDtypeStruct((rows, columns), jnp.bfloat16),
        2 * rows * depth * columns,
        2 * depth * columns + 2 * rows * (depth + columns),
        grid=(columns // tile,),
        in_specs=[pl.BlockSpec((rows, width), lambda j: (0, 0))] * len(pieces)
        + [pl.BlockSpec((depth, tile), lambda j: (0, j))],
        out_specs=pl.BlockSpec((rows, tile), lambda j: (0, j)),
    )(*pieces, in_hbm(out_proj))


def layer(
    pool_input,
    group_mix,
    group_scale,
    out_proj,
    moe_input,
    norm_gain,
    expert_ids,
    expert_scores,
    gate_proj,
    up_proj,
    down_proj,
):
    n_half, n_inner, n_tp = (lax.axis_size(axis) for axis in ("half", "inner", "tp"))
    tokens, width = moe_input.shape
    members = n_inner * n_tp
    experts = n_half * members
    capacity = 2 * tokens * expert_ids.shape[1] // experts
    slots = members * capacity
    pool_rows = pool_input.shape[0]

    def across(value):
        return lax.ppermute(value, "half", [(0, 1), (1, 0)])

    def spread(rows):
        out = lax.all_to_all(
            rows.reshape(members, capacity, width), ("inner", "tp"), 0, 0, tiled=True
        )
        return out.reshape(slots, width)

    halo = lax.ppermute(
        pool_input[pool_rows - HALO :],
        ("half", "inner"),
        [(source, source + 1) for source in range(n_half * n_inner - 1)],
    )
    normed = norm_rows(moe_input, norm_gain)
    other_rows = across(normed)
    meta, own_slots = route(expert_ids, expert_scores, normed, capacity, experts, slots)
    other_meta = across(meta)
    own_in = spread(own_slots)

    hidden = pool(halo, pool_input, group_mix, group_scale, n_tp)
    pieces = [hidden[0]] + [
        lax.ppermute(hidden[step], "tp", [(s, peer(s, step, n_tp)) for s in range(n_tp)])
        for step in range(1, n_tp)
    ]
    other_rows, own_in = lax.optimization_barrier((other_rows, own_in))
    other_slots = pick(other_meta, other_rows, slots)
    other_in = spread(other_slots)
    own_out = experts_on(own_in, gate_proj, up_proj, down_proj)
    own_out, other_in = lax.optimization_barrier((own_out, other_in))
    other_out = experts_on(other_in, gate_proj, up_proj, down_proj)
    other_back = spread(other_out)
    mixed_tokens = project(pieces, out_proj)
    mixed_tokens, other_back = lax.optimization_barrier((mixed_tokens, other_back))
    partial = combine(other_meta, other_back)
    own_out, partial = lax.optimization_barrier((own_out, partial))
    partial_back = across(partial)
    own_back = spread(own_out)
    mixed_experts = combine(meta, own_back, partial_back)
    return (mixed_tokens, mixed_experts)


def solution(mesh):
    n_ep, n_tp = mesh.shape["ep"], mesh.shape["tp"]
    split = Mesh(mesh.devices.reshape(2, n_ep // 2, n_tp), ("half", "inner", "tp"))
    ep = ("half", "inner")
    every = ("half", "inner", "tp")
    placed = (
        P(ep, "tp"),
        P("tp", None, None),
        P("tp"),
        P(),
        P(every, None),
        P(),
        P(every, None),
        P(every, None),
        P(every, None, None),
        P(every, None, None),
        P(every, None, None),
    )
    return jax.shard_map(
        layer,
        mesh=split,
        in_specs=placed,
        out_specs=(P(every, None), P(every, None)),
        check_vma=False,
    )
```
